32 devices in a mesh: sp: 8 (over z, y), tp: 4 (over x, core).
Axes of the slice: x: 2, y: 2, z: 4, core: 2. Of those that a mesh axis runs over, the one named last changes fastest.
Arguments:
- tokens: bfloat16 [6144, 2048], P('sp', 'tp'), may hold values from -18 to 18
- proj_weight: bfloat16 [2048, 1024], P(None, 'tp'), may hold values from -0.125 to 0.125
- gate_weight: bfloat16 [2048, 1024], P(None, 'tp'), may hold values from -0.125 to 0.125
- conv_weight: float32 [4, 1024], replicated, may hold values from -3 to 3
- recur_weight: bfloat16 [16, 64, 64], replicated, may hold values from -0.75 to 0.75
- input_weight: bfloat16 [16, 64, 64], replicated, may hold values from -0.75 to 0.75
- decay_param: float32 [1024], replicated, as said below
- out_grad: bfloat16 [6144, 1024], P('sp', 'tp'), may hold values from -6 to 6
Outputs:
- d_proj: bfloat16 [6144, 1024], P('sp', 'tp')
- d_gate: bfloat16 [6144, 1024], P('sp', 'tp')
- d_weight: float32 [2048, 1024], P('sp', 'tp')
The draws below stay inside these ranges and needn't reach their ends.
Inputs may be any that keep to these rules, and one draw needn't show every extreme that they name: `decay_param`: every channel's decay parameter is at least 4; there is no fixed upper bound.
All inputs are finite; a program needn't handle non-finite values.
Results may differ from the reference program's by a relative error of at most 0.01.
Values may be sent and summed in bfloat16 or wider, within the bound.
A program may use at most 64 MiB of HBM per device.

```python
import jax
import jax.numpy as jnp
from jax import lax

D = 2048
CHANNELS = 1024
BLOCK = 64
TOK_DEV = 768
TOKENS = 6144


def draw_tokens(key, part):
    key_base = jax.random.fold_in(key, 11)
    key_scale = jax.random.fold_in(key, 12)
    base = jnp.clip(jax.random.normal(key_base, (TOKENS, D), jnp.float32), -6.0, 6.0)
    span_count = TOKENS // TOK_DEV
    scales = jnp.exp(jax.random.uniform(key_scale, (span_count, 1, 1), jnp.float32, jnp.log(0.4), jnp.log(2.5)))
    shaped = base.reshape(span_count, TOK_DEV, D) * scales
    return shaped.reshape(TOKENS, D).astype(jnp.bfloat16)


def draw_decay_param(key, part):
    key_pick = jax.random.fold_in(key, 21)
    key_slow = jax.random.fold_in(key, 22)
    key_fast = jax.random.fold_in(key, 23)
    slow_pick = jax.random.randint(key_pick, (CHANNELS,), 0, 2) > 0
    slow_value = jnp.log(jnp.float32(TOKENS)) + jax.random.uniform(key_slow, (CHANNELS,), jnp.float32, 0.7, 2.2)
    fast_value = jax.random.uniform(key_fast, (CHANNELS,), jnp.float32, 4.4, 5.3)
    return jnp.where(slow_pick, slow_value, fast_value).astype(jnp.float32)


def block_levels(rng, dims, shards, smallest, largest):
    gain, own = 1.0, jax.random.fold_in(rng, 6)
    for axis_at, blocks in shards:
        steps = jnp.exp(jax.random.uniform(jax.random.fold_in(own, axis_at), (blocks,), jnp.float32, smallest / len(shards), largest / len(shards)))
        gain = gain * jnp.repeat(steps, dims[axis_at] // blocks).reshape([-1 if axis == axis_at else 1 for axis in range(len(dims))])
    return gain


def gaussian(own_key, dims, deviation, reach, shards=(), kind=jnp.bfloat16):
    gain = block_levels(own_key, dims, shards, -0.22, 0.18) if shards else 1.0
    entries = jax.random.normal(own_key, dims, jnp.float32) * deviation * gain
    return jnp.minimum(jnp.maximum(entries, -reach), reach).astype(kind)


def setup_inputs(seed: int = 0) -> dict:
    key_list = jax.random.split(jax.random.key(seed), 9)
    tokens = draw_tokens(jax.random.fold_in(key_list[8], 71), 0)
    proj_weight = gaussian(key_list[1], (D, CHANNELS), D ** -0.5, 0.125, ((1, 4),))
    gate_weight = gaussian(key_list[2], (D, CHANNELS), D ** -0.5, 0.125, ((1, 4),))
    conv_weight = gaussian(key_list[3], (4, CHANNELS), 4 ** -0.5, 3.0, (), jnp.float32)
    recur_weight = gaussian(key_list[4], (CHANNELS // BLOCK, BLOCK, BLOCK), BLOCK ** -0.5, 0.75)
    input_weight = gaussian(key_list[5], (CHANNELS // BLOCK, BLOCK, BLOCK), BLOCK ** -0.5, 0.75)
    decay_param = draw_decay_param(jax.random.fold_in(key_list[8], 71), 0)
    out_grad = gaussian(key_list[7], (TOKENS, CHANNELS), 1.0, 6.0, ((0, 8), (1, 4)))
    return dict(tokens=tokens, proj_weight=proj_weight, gate_weight=gate_weight, conv_weight=conv_weight, recur_weight=recur_weight, input_weight=input_weight, decay_param=decay_param, out_grad=out_grad)


rate_scale = 8.0
scale_floor = 0.0001

def combine(earlier, later):
    return (earlier[0] * later[0], later[0] * earlier[1] + later[1])

def reference(tokens, proj_weight, gate_weight, conv_weight, recur_weight, input_weight, decay_param, out_grad):
    seq_rows = tokens.shape[0]
    group_count = proj_weight.shape[1] // BLOCK

    def per_block(group):
        cols = (group * BLOCK).astype(jnp.int32)
        w_proj = lax.dynamic_slice_in_dim(proj_weight, cols, BLOCK, 1)
        w_gate = lax.dynamic_slice_in_dim(gate_weight, cols, BLOCK, 1)
        conv_taps = lax.dynamic_slice_in_dim(conv_weight, cols, BLOCK, 1)
        decay_slice = lax.dynamic_slice_in_dim(decay_param, cols, BLOCK, 0)
        w_recur = lax.dynamic_index_in_dim(recur_weight, group.astype(jnp.int32), 0, False)
        w_input = lax.dynamic_index_in_dim(input_weight, group.astype(jnp.int32), 0, False)
        cotangent = lax.dynamic_slice_in_dim(out_grad, cols, BLOCK, 1).astype(jnp.float32)
        projected = jnp.dot(tokens, w_proj, preferred_element_type=jnp.float32).astype(jnp.bfloat16)
        gate_in = jnp.dot(tokens, w_gate, preferred_element_type=jnp.float32).astype(jnp.bfloat16)
        padded = jnp.concatenate([jnp.zeros((3, BLOCK), jnp.float32), projected.astype(jnp.float32)], axis=0)
        total = conv_taps[0] * padded[3:3 + seq_rows]
        for offset in range(1, 4):
            total = total + conv_taps[offset] * padded[3 - offset:3 - offset + seq_rows]
        conv_out = total.astype(jnp.bfloat16)
        conv_float = conv_out.astype(jnp.float32)
        recur_pre = jnp.dot(conv_out, w_recur, preferred_element_type=jnp.float32)
        input_pre = jnp.dot(conv_out, w_input, preferred_element_type=jnp.float32)
        recur_open = jax.nn.sigmoid(recur_pre)
        input_open = jax.nn.sigmoid(input_pre)
        log_slope = rate_scale * jax.nn.log_sigmoid(decay_slice)
        log_decay = log_slope * recur_open
        decay_rate = jnp.exp(log_decay)
        input_scale = jnp.sqrt(scale_floor - jnp.expm1(2.0 * log_decay))
        gated_input = input_open * conv_float
        drive = input_scale * gated_input
        _, states = lax.associative_scan(combine, (decay_rate, drive), axis=0)
        previous = jnp.concatenate([jnp.zeros((1, BLOCK), jnp.float32), states[:-1]], axis=0)
        gelu_gate, gelu_back = jax.vjp(jax.nn.gelu, gate_in.astype(jnp.float32))
        d_gate = gelu_back(cotangent * states)[0].astype(jnp.bfloat16)
        drive_grad = cotangent * gelu_gate
        shifted = jnp.concatenate([decay_rate[1:], jnp.ones((1, BLOCK), jnp.float32)], axis=0)
        _, state_grad = lax.associative_scan(combine, (shifted, drive_grad), reverse=True, axis=0)
        d_log_decay = state_grad * (decay_rate * previous - gated_input * decay_rate * decay_rate / input_scale)
        d_recur_pre = (d_log_decay * log_slope * recur_open * (1.0 - recur_open)).astype(jnp.bfloat16)
        d_input_pre = (state_grad * input_scale * conv_float * input_open * (1.0 - input_open)).astype(jnp.bfloat16)
        d_conv = state_grad * input_scale * input_open
        d_conv = d_conv + jnp.dot(d_recur_pre, w_recur.T, preferred_element_type=jnp.float32)
        d_conv = d_conv + jnp.dot(d_input_pre, w_input.T, preferred_element_type=jnp.float32)
        extended = jnp.concatenate([d_conv, jnp.zeros((3, BLOCK), jnp.float32)], axis=0)
        grad_sum = conv_taps[0] * extended[0:seq_rows]
        for offset in range(1, 4):
            grad_sum = grad_sum + conv_taps[offset] * extended[offset:offset + seq_rows]
        d_proj = grad_sum.astype(jnp.bfloat16)
        d_weight = lax.dot_general(tokens, d_proj, (((0,), (0,)), ((), ())), preferred_element_type=jnp.float32)
        return (d_proj, d_gate, d_weight)
    d_proj, d_gate, d_weight = lax.map(per_block, jnp.arange(group_count, dtype=jnp.int32))
    d_proj = jnp.transpose(d_proj, (1, 0, 2)).reshape(seq_rows, group_count * BLOCK)
    d_gate = jnp.transpose(d_gate, (1, 0, 2)).reshape(seq_rows, group_count * BLOCK)
    d_weight = jnp.transpose(d_weight, (1, 0, 2)).reshape(d_weight.shape[1], group_count * BLOCK)
    return (d_proj, d_gate, d_weight)
```

```python
import functools

import jax
import jax.numpy as jnp
from jax import lax
from jax.experimental import pallas as pl
from jax.experimental.pallas import tpu as pltpu
from jax.sharding import PartitionSpec as P

BLOCK = 64
rate_scale = 8.0
scale_floor = 0.0001

SUBS = 8
STEP = 16
LANES = 128
PAD = 8
MESH = pl.DeviceIdType.MESH
F32 = jnp.float32
BF16 = jnp.bfloat16


def mm(a, b, dims=(((1,), (0,)), ((), ()))):
    return lax.dot_general(a, b, dims, preferred_element_type=F32)


def kernel(
    tok_hbm, wp_hbm, wg_hbm, cw_ref, wr_ref, wi_ref, dp_ref, og_hbm,
    dproj_ref, dgate_ref, dw_ref,
    gath, wp, wg, og, wblk, proj, gin, pre,
    dec, drv, dgr, qg, ro_s, io_s, cv_s, sc_s, rs_s, xp, cp, gs, as_,
    ends, carry_k, carry_l, slope_s, taps_s,
    halo_out, halo_in, car_out, car_in, dri, dc, dc_in, dpt, sbuf, rbuf, own,
    loc_sem, ag_send, ag_recv, halo_send, halo_recv, car_send, car_recv,
    dc_send, dc_recv, rs_send, rs_recv,
    *, sp_n, tp_n,
):
    sp = lax.axis_index("sp")
    tp = lax.axis_index("tp")
    core = lax.rem(tp, 2)
    chip = lax.div(tp, 2)
    chips = tp_n // 2
    partner = tp + 1 - 2 * core
    sub_rows = gath.shape[2]
    feat = gath.shape[3]
    chan = wp.shape[1]
    halves = chan // LANES
    pitch = sub_rows + PAD
    chunks = sub_rows // STEP
    rows = SUBS * sub_rows
    groups = chan // BLOCK

    loc = [
        pltpu.make_async_copy(tok_hbm, gath.at[0], loc_sem.at[0]),
        pltpu.make_async_copy(wp_hbm, wp, loc_sem.at[1]),
        pltpu.make_async_copy(wg_hbm, wg, loc_sem.at[2]),
        pltpu.make_async_copy(og_hbm, og, loc_sem.at[3]),
    ]
    for item in loc:
        item.start()

    def sp_at(j):
        return lax.rem(sp + j, sp_n)

    def chip_at(j):
        return lax.rem(chip + j, chips)

    barrier = pltpu.get_barrier_semaphore()
    pl.semaphore_signal(barrier, inc=1, device_id=(sp, partner), device_id_type=MESH)
    for j in range(1, chips):
        pl.semaphore_signal(
            barrier, inc=1, device_id=(sp, chip_at(j) * 2 + core), device_id_type=MESH
        )

    def greet(j, _):
        pl.semaphore_signal(barrier, inc=1, device_id=(sp_at(j), tp), device_id_type=MESH)
        return 0

    lax.fori_loop(1, sp_n, greet, 0)

    cols = pl.ds(pl.multiple_of(tp * chan, chan), chan)
    z = jnp.exp(-dp_ref[:, cols])
    log1p = z * (1.0 - z * (1.0 / 2 - z * (1.0 / 3 - z * (1.0 / 4 - z * (1.0 / 5)))))
    slope_s[...] = -rate_scale * log1p
    taps_s[...] = cw_ref[:, cols]
    wblk[...] = jnp.zeros_like(wblk)
    for g in range(groups):
        at = slice(g * BLOCK, (g + 1) * BLOCK)
        wblk[at, at] = wr_ref[tp * groups + g]
        wblk[at, chan + g * BLOCK : chan + (g + 1) * BLOCK] = wi_ref[tp * groups + g]

    pl.semaphore_wait(barrier, chips + sp_n - 1)
    loc[0].wait()

    def part(c):
        return pl.ds(pl.multiple_of(c * STEP, STEP), STEP)

    def ag_copy(slot, source, c, target):
        return pltpu.make_async_remote_copy(
            src_ref=gath.at[source, :, part(c), :],
            dst_ref=gath.at[slot, :, part(c), :],
            send_sem=ag_send.at[slot, c],
            recv_sem=ag_recv.at[slot, c],
            device_id=(sp, target),
            device_id_type=MESH,
        )

    def cross(j, c):
        return ag_copy(2 * j, 0, c, chip_at(j) * 2 + core)

    def inside(j, c):
        return ag_copy(2 * j + 1, 2 * j, c, partner)

    def send_own(k, _):
        c = lax.rem(k + chunks - 1, chunks)
        for j in range(1, chips):
            cross(j, c).start()
        inside(0, c).start()
        return 0

    lax.fori_loop(0, chunks, send_own, 0)
    for item in loc[1:]:
        item.wait()

    def relay(c):
        for j in range(1, chips):
            cross(j, c).wait_recv()
            inside(j, c).start()

    def project(c):
        acc_p = acc_g = None
        for j in range(chips):
            for other in range(2):
                rel = 2 * j + other
                if other:
                    inside(j, c).wait_recv()
                shard = lax.rem(chip + chips - j, chips) * 2 + (1 - core if other else core)
                x = gath[rel, :, part(c), :].reshape(SUBS * STEP, feat)
                wrows = pl.ds(pl.multiple_of(shard * feat, feat), feat)
                a = mm(x, wp[wrows, :])
                b = mm(x, wg[wrows, :])
                acc_p = a if acc_p is None else acc_p + a
                acc_g = b if acc_g is None else acc_g + b
        shape = (SUBS, STEP, chan)
        proj[:, pl.ds(pl.multiple_of(c * STEP + PAD, PAD), STEP), :] = (
            acc_p.astype(BF16).astype(F32).reshape(shape)
        )
        gin[:, part(c), :] = acc_g.astype(BF16).astype(F32).reshape(shape)

    def gates(c):
        def conv(s, _):
            x = proj[s, pl.ds(pl.multiple_of(c * STEP, PAD), STEP + PAD), :]
            total = taps_s[0:1, :] * x[PAD:]
            for k in range(1, 4):
                total = total + taps_s[k : k + 1, :] * pltpu.roll(x, k, 0)[PAD:]
            dri[pl.ds(pl.multiple_of(s * STEP, STEP), STEP), 0:chan] = total.astype(BF16)
            return 0

        lax.fori_loop(0, SUBS, conv, 0, unroll=4)
        pre[...] = mm(dri[0 : SUBS * STEP, 0:chan], wblk[...])

        def element(s, _):
            at = pl.ds(pl.multiple_of(s * STEP, STEP), STEP)
            to = pl.ds(pl.multiple_of(s * pitch + c * STEP, PAD), STEP)
            src = pl.ds(pl.multiple_of(s * sub_rows + c * STEP, STEP), STEP)
            for h in range(halves):
                lane = slice(h * LANES, (h + 1) * LANES)
                slope = slope_s[:, lane]
                cv = dri[at, lane].astype(F32)
                ro = 0.5 * jnp.tanh(0.5 * pre[at, lane]) + 0.5
                io = 0.5 * jnp.tanh(0.5 * pre[at, chan + h * LANES : chan + (h + 1) * LANES]) + 0.5
                ld = slope * ro
                d = jnp.exp(ld)
                y = 2.0 * ld
                poly = 1.0 + y * (1.0 / 8)
                for m in range(7, 1, -1):
                    poly = 1.0 + (y * (1.0 / m)) * poly
                u = scale_floor - y * poly
                rs = lax.rsqrt(u)
                sc = u * rs
                x = gin[s, part(c), lane]
                cot = og[src, lane].astype(F32)
                x2 = x * x
                th = jnp.tanh(0.7978845608028654 * (x + 0.044715 * (x2 * x)))
                half_up = 0.5 * (1.0 + th)
                slope_g = half_up + 0.5 * x * (1.0 - th * th) * (
                    0.7978845608028654 * (1.0 + 0.134145 * x2)
                )
                dec[h, to, :] = d
                drv[h, to, :] = sc * (io * cv)
                dgr[h, to, :] = cot * (x * half_up)
                qg[h, to, :] = cot * slope_g
                ro_s[h, to, :] = ro
                io_s[h, to, :] = io
                cv_s[h, to, :] = cv
                sc_s[h, to, :] = sc
                rs_s[h, to, :] = rs
            return 0

        lax.fori_loop(0, SUBS, element, 0, unroll=4)

    halo = pltpu.make_async_remote_copy(
        src_ref=halo_out, dst_ref=halo_in, send_sem=halo_send, recv_sem=halo_recv,
        device_id=(sp_at(1), tp), device_id_type=MESH,
    )
    relay(chunks - 1)
    project(chunks - 1)
    halo_out[...] = proj[SUBS - 1, sub_rows:pitch, :]
    halo.start()
    for s in range(1, SUBS):
        proj[s, 0:PAD, :] = proj[s - 1, sub_rows:pitch, :]
    relay(0)
    project(0)
    halo.wait()
    proj[0, 0:PAD, :] = jnp.where(sp > 0, halo_in[...], 0.0)

    def stream(c, _):
        relay(c)
        gates(c - 1)
        project(c)
        return 0

    lax.fori_loop(1, chunks - 1, stream, 0)

    def rest(c, _):
        gates(c)
        return 0

    lax.fori_loop(chunks - 2, chunks, rest, 0)

    one = jnp.ones((SUBS, LANES), F32)
    zero = jnp.zeros((SUBS, LANES), F32)

    def scan(i, state):
        out = []
        fwd = pl.ds(i, SUBS, stride=pitch)
        rev = pl.ds(sub_rows - 1 - i, SUBS, stride=pitch)
        for h in range(halves):
            x, c, g, a = state[4 * h : 4 * h + 4]
            d = dec.at[h][fwd, :]
            xp.at[h][fwd, :] = x
            cp.at[h][fwd, :] = c
            x = d * x + drv.at[h][fwd, :]
            c = c * d
            e = dec.at[h][rev, :]
            g = g + dgr.at[h][rev, :]
            gs.at[h][rev, :] = g
            as_.at[h][rev, :] = a
            g = e * g
            a = a * e
            out += [x, c, g, a]
        return tuple(out)

    final = lax.fori_loop(0, sub_rows, scan, (zero, one, zero, one) * halves, unroll=4)
    for h in range(halves):
        lane = slice(h * LANES, (h + 1) * LANES)
        ends[0, :, lane] = final[4 * h + 1]
        ends[1, :, lane] = final[4 * h]
        ends[2, :, lane] = final[4 * h + 2]
    p_list, q_list, b_list, e_list = [], [], [None] * SUBS, [None] * SUBS
    p = jnp.zeros((1, chan), F32)
    q = jnp.ones((1, chan), F32)
    for s in range(SUBS):
        p_list.append(p)
        q_list.append(q)
        p = ends[0, s : s + 1, :] * p + ends[1, s : s + 1, :]
        q = ends[0, s : s + 1, :] * q
    b = jnp.zeros((1, chan), F32)
    e = jnp.ones((1, chan), F32)
    for s in range(SUBS - 1, -1, -1):
        b_list[s] = b
        e_list[s] = e
        b = ends[0, s : s + 1, :] * b + ends[2, s : s + 1, :]
        e = ends[0, s : s + 1, :] * e
    car_out[0:1, :] = q
    car_out[1:2, :] = p
    car_out[2:3, :] = b
    car_out[3:8, :] = jnp.zeros((5, chan), F32)

    def car_copy(j):
        return pltpu.make_async_remote_copy(
            src_ref=car_out, dst_ref=car_in.at[j], send_sem=car_send.at[j],
            recv_sem=car_recv.at[j], device_id=(sp_at(j), tp), device_id_type=MESH,
        )

    def car_start(j, _):
        car_copy(j).start()
        return 0

    def car_wait(j, _):
        car_copy(j).wait()
        return 0

    lax.fori_loop(1, sp_n, car_start, 0)
    lax.fori_loop(1, sp_n, car_wait, 0)

    def join(m, state):
        cs, cg = state
        j = sp_n - m
        cs = jnp.where(j <= sp, car_in[j, 0:1, :] * cs + car_in[j, 1:2, :], cs)
        cg = jnp.where(sp + j < sp_n, car_in[m, 0:1, :] * cg + car_in[m, 2:3, :], cg)
        return cs, cg

    nothing = jnp.zeros((1, chan), F32)
    cs, cg = lax.fori_loop(1, sp_n, join, (nothing, nothing))
    for s in range(SUBS):
        carry_k[s] = p_list[s] + q_list[s] * cs
        carry_l[s] = b_list[s] + e_list[s] * cg

    def back(s):
        base = pl.multiple_of(s * pitch, PAD)
        outb = pl.multiple_of(s * sub_rows, STEP)
        for r in range(0, sub_rows, STEP):
            at = pl.ds(base + r, STEP)
            to = pl.ds(outb + r, STEP)
            for h in range(halves):
                lane = slice(h * LANES, (h + 1) * LANES)
                kk = carry_k[s, :, lane]
                ll = carry_l[s, :, lane]
                d = dec[h, at, :]
                prev = xp[h, at, :] + cp[h, at, :] * kk
                dp = d * prev
                dgate_ref[to, lane] = (qg[h, at, :] * (dp + drv[h, at, :])).astype(BF16)
                sg = gs[h, at, :] + as_[h, at, :] * ll
                ro, io, cv, sc = ro_s[h, at, :], io_s[h, at, :], cv_s[h, at, :], sc_s[h, at, :]
                dld = sg * (dp - io * cv * d * d * rs_s[h, at, :])
                dr = dld * slope_s[:, lane] * ro * (1.0 - ro)
                sgi = sg * sc * io
                di = sgi * cv * (1.0 - io)
                dri[r : r + STEP, lane] = dr.astype(BF16)
                dri[r : r + STEP, chan + h * LANES : chan + (h + 1) * LANES] = di.astype(BF16)
                dc[to, lane] = sgi
        whole = pl.ds(outb, sub_rows)
        dc[whole, :] += mm(dri[0:sub_rows, :], wblk[...], (((1,), (1,)), ((), ())))

    back(0)
    halo_out[...] = dc[0:PAD, :]
    dc_copy = pltpu.make_async_remote_copy(
        src_ref=halo_out, dst_ref=dc_in, send_sem=dc_send, recv_sem=dc_recv,
        device_id=(sp_at(sp_n - 1), tp), device_id_type=MESH,
    )
    dc_copy.start()

    def back_step(s, _):
        back(s)
        return 0

    lax.fori_loop(1, SUBS, back_step, 0)
    dc_copy.wait()
    dc[rows : rows + PAD, :] = jnp.where(sp < sp_n - 1, dc_in[...], 0.0)

    def unconv(i, _):
        r = pl.multiple_of(i * STEP, STEP)
        x = dc[pl.ds(r, STEP + PAD), :]
        total = taps_s[0:1, :] * x[:STEP]
        for k in range(1, 4):
            total = total + taps_s[k : k + 1, :] * pltpu.roll(x, STEP + PAD - k, 0)[:STEP]
        dproj_ref[pl.ds(r, STEP), :] = total.astype(BF16)
        return 0

    lax.fori_loop(0, rows // STEP, unconv, 0, unroll=4)

    piece = feat * tp_n // sp_n
    flip = piece % LANES == 0

    def rs_copy(j):
        return pltpu.make_async_remote_copy(
            src_ref=sbuf.at[j if flip else sp_at(j)], dst_ref=rbuf.at[j],
            send_sem=rs_send.at[j], recv_sem=rs_recv.at[j],
            device_id=(sp_at(j), tp), device_id_type=MESH,
        )

    def slot_of(shard):
        behind = lax.rem(chip + chips - lax.div(shard, 2), chips)
        return 2 * behind + lax.rem(lax.rem(shard, 2) + core, 2)

    if flip:
        dpt[...] = dproj_ref[...].T
        per = feat // piece

        def share(j):
            dest = sp_at(j)
            x = gath[
                slot_of(lax.div(dest, per)), :, :,
                pl.ds(pl.multiple_of(lax.rem(dest, per) * piece, LANES), piece),
            ]
            return mm(dpt[...], x.reshape(rows, piece))

        def rs_start(j, _):
            sbuf[j] = share(j).astype(BF16)
            rs_copy(j).start()
            return 0

        lax.fori_loop(1, sp_n, rs_start, 0)
        own[...] = share(0)
    else:
        per = feat // piece

        def shares(shard, _):
            x = gath[slot_of(shard)].reshape(rows, feat)
            full = mm(x, dproj_ref[...], (((0,), (0,)), ((), ())))
            sbuf[pl.ds(shard * per, per)] = full.astype(BF16).reshape(per, piece, chan)
            return 0

        lax.fori_loop(0, tp_n, shares, 0)

        def rs_start(j, _):
            rs_copy(j).start()
            return 0

        lax.fori_loop(1, sp_n, rs_start, 0)
        own[...] = sbuf[sp].astype(F32)

    def ag_drain(c, _):
        for j in range(chips):
            if j:
                cross(j, c).wait_send()
            inside(j, c).wait_send()
        return 0

    lax.fori_loop(0, chunks, ag_drain, 0)

    def rs_wait(j, _):
        rs_copy(j).wait()
        return 0

    lax.fori_loop(1, sp_n, rs_wait, 0)
    height = own.shape[0]
    tile = min(32, height)

    def add(i, _):
        at = pl.ds(pl.multiple_of(i * tile, tile), tile)

        def more(j, acc):
            return acc + rbuf[j, at, :].astype(F32)

        own[at, :] = lax.fori_loop(1, sp_n, more, own[at, :])
        return 0

    lax.fori_loop(0, height // tile, add, 0)
    dw_ref[...] = own[...].T if flip else own[...]


def per_device(
    tokens, proj_weight, gate_weight, conv_weight, recur_weight, input_weight, decay_param, out_grad
):
    sp_n = lax.axis_size("sp")
    tp_n = lax.axis_size("tp")
    rows, feat = tokens.shape
    width, chan = proj_weight.shape
    sub_rows = rows // SUBS
    chunks = sub_rows // STEP
    halves = chan // LANES
    pitch = sub_rows + PAD
    piece = width // sp_n
    box = (chan, piece) if piece % LANES == 0 else (piece, chan)
    V = pltpu.VMEM
    DMA = pltpu.SemaphoreType.DMA
    tall = V((halves, SUBS * pitch, LANES), F32)
    small = V((PAD, chan), F32)
    any_space = pl.BlockSpec(memory_space=pl.ANY)
    in_vmem = pl.BlockSpec(memory_space=V)
    return pl.pallas_call(
        functools.partial(kernel, sp_n=sp_n, tp_n=tp_n),
        out_shape=(
            jax.ShapeDtypeStruct((rows, chan), BF16),
            jax.ShapeDtypeStruct((rows, chan), BF16),
            jax.ShapeDtypeStruct((piece, chan), F32),
        ),
        in_specs=[any_space] * 3 + [in_vmem] * 4 + [any_space],
        out_specs=(in_vmem,) * 3,
        scratch_shapes=[
            V((tp_n, SUBS, sub_rows, feat), BF16),
            V((width, chan), BF16),
            V((width, chan), BF16),
            V((rows, chan), BF16),
            V((chan, 2 * chan), BF16),
            V((SUBS, pitch, chan), F32),
            V((SUBS, sub_rows, chan), F32),
            V((SUBS * STEP, 2 * chan), F32),
        ] + [tall] * 13 + [
            V((3, SUBS, chan), F32),
            V((SUBS, 1, chan), F32),
            V((SUBS, 1, chan), F32),
            V((1, chan), F32),
            V((4, chan), F32),
            small,
            small,
            small,
            V((sp_n, PAD, chan), F32),
            V((max(SUBS * STEP, sub_rows), 2 * chan), BF16),
            V((rows + PAD, chan), F32),
            small,
            V((chan, rows), BF16),
            V((sp_n,) + box, BF16),
            V((sp_n,) + box, BF16),
            V(box, F32),
            DMA((4,)),
            DMA((tp_n, chunks)), DMA((tp_n, chunks)),
            DMA, DMA,
            DMA((sp_n,)), DMA((sp_n,)),
            DMA, DMA,
            DMA((sp_n,)), DMA((sp_n,)),
        ],
        compiler_params=pltpu.CompilerParams(
            collective_id=0, has_side_effects=True, vmem_limit_bytes=56 * 1024 * 1024
        ),
    )(
        tokens.reshape(SUBS, sub_rows, feat), proj_weight, gate_weight, conv_weight,
        recur_weight, input_weight, decay_param.reshape(1, -1), out_grad,
    )


def solution(mesh):
    in_specs = (P("sp", "tp"), P(None, "tp"), P(None, "tp"), P(), P(), P(), P(), P("sp", "tp"))
    out_specs = (P("sp", "tp"), P("sp", "tp"), P("sp", "tp"))
    return jax.shard_map(
        per_device, mesh=mesh, in_specs=in_specs, out_specs=out_specs, check_vma=False
    )
```

```python
import functools

import jax
import jax.numpy as jnp
from jax import lax
from jax.experimental import pallas as pl
from jax.experimental.pallas import tpu as pltpu
from jax.sharding import PartitionSpec as P

BLOCK = 64
rate_scale = 8.0
scale_floor = 0.0001

SUBS = 8
STEP = 16
LANES = 128
PAD = 8
MESH = pl.DeviceIdType.MESH
F32 = jnp.float32
BF16 = jnp.bfloat16


def mm(a, b, dims=(((1,), (0,)), ((), ()))):
    return lax.dot_general(a, b, dims, preferred_element_type=F32)


def kernel(
    tok_hbm, wp_hbm, wg_hbm, cw_ref, wr_ref, wi_ref, dp_ref, og_hbm,
    dproj_ref, dgate_ref, dw_ref,
    gath, wp, wg, og, wblk, proj, gin, pre,
    dec, drv, dgr, qg, ro_s, io_s, cv_s, sc_s, rs_s, xp, cp, gs, as_,
    ends, carry_k, carry_l, slope_s, taps_s,
    halo_out, halo_in, car_out, car_in, dri, dc, dc_in, dpt, sbuf, rbuf, own,
    loc_sem, ag_send, ag_recv, halo_send, halo_recv, car_send, car_recv,
    dc_send, dc_recv, rs_send, rs_recv,
    *, sp_n, tp_n,
):
    sp = lax.axis_index("sp")
    tp = lax.axis_index("tp")
    core = lax.rem(tp, 2)
    chip = lax.div(tp, 2)
    chips = tp_n // 2
    partner = tp + 1 - 2 * core
    sub_rows = gath.shape[2]
    feat = gath.shape[3]
    chan = wp.shape[1]
    halves = chan // LANES
    pitch = sub_rows + PAD
    chunks = sub_rows // STEP
    rows = SUBS * sub_rows
    groups = chan // BLOCK

    loc = [
        pltpu.make_async_copy(tok_hbm, gath.at[0], loc_sem.at[0]),
        pltpu.make_async_copy(wp_hbm, wp, loc_sem.at[1]),
        pltpu.make_async_copy(wg_hbm, wg, loc_sem.at[2]),
        pltpu.make_async_copy(og_hbm, og, loc_sem.at[3]),
    ]
    for item in loc:
        item.start()

    def sp_at(j):
        return lax.rem(sp + j, sp_n)

    def chip_at(j):
        return lax.rem(chip + j, chips)

    barrier = pltpu.get_barrier_semaphore()
    pl.semaphore_signal(barrier, inc=1, device_id=(sp, partner), device_id_type=MESH)
    for j in range(1, chips):
        pl.semaphore_signal(
            barrier, inc=1, device_id=(sp, chip_at(j) * 2 + core), device_id_type=MESH
        )

    def greet(j, _):
        pl.semaphore_signal(barrier, inc=1, device_id=(sp_at(j), tp), device_id_type=MESH)
        return 0

    lax.fori_loop(1, sp_n, greet, 0)

    cols = pl.ds(pl.multiple_of(tp * chan, chan), chan)
    z = jnp.exp(-dp_ref[:, cols])
    log1p = z * (1.0 - z * (1.0 / 2 - z * (1.0 / 3 - z * (1.0 / 4 - z * (1.0 / 5)))))
    slope_s[...] = -rate_scale * log1p
    taps_s[...] = cw_ref[:, cols]
    wblk[...] = jnp.zeros_like(wblk)
    for g in range(groups):
        at = slice(g * BLOCK, (g + 1) * BLOCK)
        wblk[at, at] = wr_ref[tp * groups + g]
        wblk[at, chan + g * BLOCK : chan + (g + 1) * BLOCK] = wi_ref[tp * groups + g]

    pl.semaphore_wait(barrier, chips + sp_n - 1)
    loc[0].wait()

    def part(c):
        return pl.ds(pl.multiple_of(c * STEP, STEP), STEP)

    def ag_copy(slot, source, c, target):
        return pltpu.make_async_remote_copy(
            src_ref=gath.at[source, :, part(c), :],
            dst_ref=gath.at[slot, :, part(c), :],
            send_sem=ag_send.at[slot, c],
            recv_sem=ag_recv.at[slot, c],
            device_id=(sp, target),
            device_id_type=MESH,
        )

    def cross(j, c):
        return ag_copy(2 * j, 0, c, chip_at(j) * 2 + core)

    def inside(j, c):
        return ag_copy(2 * j + 1, 2 * j, c, partner)

    def send_own(k, _):
        c = lax.rem(k + chunks - 1, chunks)
        for j in range(1, chips):
            cross(j, c).start()
        inside(0, c).start()
        return 0

    lax.fori_loop(0, chunks, send_own, 0)
    for item in loc[1:]:
        item.wait()

    def relay(c):
        for j in range(1, chips):
            cross(j, c).wait_recv()
            inside(j, c).start()

    def project(c):
        acc_p = acc_g = None
        for j in range(chips):
            for other in range(2):
                rel = 2 * j + other
                if other:
                    inside(j, c).wait_recv()
                shard = lax.rem(chip + chips - j, chips) * 2 + (1 - core if other else core)
                x = gath[rel, :, part(c), :].reshape(SUBS * STEP, feat)
                wrows = pl.ds(pl.multiple_of(shard * feat, feat), feat)
                a = mm(x, wp[wrows, :])
                b = mm(x, wg[wrows, :])
                acc_p = a if acc_p is None else acc_p + a
                acc_g = b if acc_g is None else acc_g + b
        shape = (SUBS, STEP, chan)
        proj[:, pl.ds(pl.multiple_of(c * STEP + PAD, PAD), STEP), :] = (
            acc_p.astype(BF16).astype(F32).reshape(shape)
        )
        gin[:, part(c), :] = acc_g.astype(BF16).astype(F32).reshape(shape)

    def gates(c):
        def conv(s, _):
            x = proj[s, pl.ds(pl.multiple_of(c * STEP, PAD), STEP + PAD), :]
            total = taps_s[0:1, :] * x[PAD:]
            for k in range(1, 4):
                total = total + taps_s[k : k + 1, :] * pltpu.roll(x, k, 0)[PAD:]
            dri[pl.ds(pl.multiple_of(s * STEP, STEP), STEP), 0:chan] = total.astype(BF16)
            return 0

        lax.fori_loop(0, SUBS, conv, 0, unroll=4)
        pre[...] = mm(dri[0 : SUBS * STEP, 0:chan], wblk[...])

        def element(s, _):
            at = pl.ds(pl.multiple_of(s * STEP, STEP), STEP)
            to = pl.ds(pl.multiple_of(s * pitch + c * STEP, PAD), STEP)
            src = pl.ds(pl.multiple_of(s * sub_rows + c * STEP, STEP), STEP)
            for h in range(halves):
                lane = slice(h * LANES, (h + 1) * LANES)
                slope = slope_s[:, lane]
                cv = dri[at, lane].astype(F32)
                ro = 0.5 * jnp.tanh(0.5 * pre[at, lane]) + 0.5
                io = 0.5 * jnp.tanh(0.5 * pre[at, chan + h * LANES : chan + (h + 1) * LANES]) + 0.5
                ld = slope * ro
                d = jnp.exp(ld)
                y = 2.0 * ld
                poly = 1.0 + y * (1.0 / 8)
                for m in range(7, 1, -1):
                    poly = 1.0 + (y * (1.0 / m)) * poly
                u = scale_floor - y * poly
                rs = lax.rsqrt(u)
                sc = u * rs
                x = gin[s, part(c), lane]
                cot = og[src, lane].astype(F32)
                x2 = x * x
                th = jnp.tanh(0.7978845608028654 * (x + 0.044715 * (x2 * x)))
                half_up = 0.5 * (1.0 + th)
                slope_g = half_up + 0.5 * x * (1.0 - th * th) * (
                    0.7978845608028654 * (1.0 + 0.134145 * x2)
                )
                dec[h, to, :] = d
                drv[h, to, :] = sc * (io * cv)
                dgr[h, to, :] = cot * (x * half_up)
                qg[h, to, :] = cot * slope_g
                ro_s[h, to, :] = ro
                io_s[h, to, :] = io
                cv_s[h, to, :] = cv
                sc_s[h, to, :] = sc
                rs_s[h, to, :] = rs
            return 0

        lax.fori_loop(0, SUBS, element, 0, unroll=4)

    halo = pltpu.make_async_remote_copy(
        src_ref=halo_out, dst_ref=halo_in, send_sem=halo_send, recv_sem=halo_recv,
        device_id=(sp_at(1), tp), device_id_type=MESH,
    )
    relay(chunks - 1)
    project(chunks - 1)
    halo_out[...] = proj[SUBS - 1, sub_rows:pitch, :]
    halo.start()
    for s in range(1, SUBS):
        proj[s, 0:PAD, :] = proj[s - 1, sub_rows:pitch, :]
    relay(0)
    project(0)
    halo.wait()
    proj[0, 0:PAD, :] = jnp.where(sp > 0, halo_in[...], 0.0)

    def stream(c, _):
        relay(c)
        gates(c - 1)
        project(c)
        return 0

    lax.fori_loop(1, chunks - 1, stream, 0)

    def rest(c, _):
        gates(c)
        return 0

    lax.fori_loop(chunks - 2, chunks, rest, 0)

    one = jnp.ones((SUBS, LANES), F32)
    zero = jnp.zeros((SUBS, LANES), F32)

    def scan(i, state):
        out = []
        fwd = pl.ds(i, SUBS, stride=pitch)
        rev = pl.ds(sub_rows - 1 - i, SUBS, stride=pitch)
        for h in range(halves):
            x, c, g, a = state[4 * h : 4 * h + 4]
            d = dec.at[h][fwd, :]
            xp.at[h][fwd, :] = x
            cp.at[h][fwd, :] = c
            x = d * x + drv.at[h][fwd, :]
            c = c * d
            e = dec.at[h][rev, :]
            g = g + dgr.at[h][rev, :]
            gs.at[h][rev, :] = g
            as_.at[h][rev, :] = a
            g = e * g
            a = a * e
            out += [x, c, g, a]
        return tuple(out)

    final = lax.fori_loop(0, sub_rows, scan, (zero, one, zero, one) * halves, unroll=4)
    for h in range(halves):
        lane = slice(h * LANES, (h + 1) * LANES)
        ends[0, :, lane] = final[4 * h + 1]
        ends[1, :, lane] = final[4 * h]
        ends[2, :, lane] = final[4 * h + 2]
    p_list, q_list, b_list, e_list = [], [], [None] * SUBS, [None] * SUBS
    p = jnp.zeros((1, chan), F32)
    q = jnp.ones((1, chan), F32)
    for s in range(SUBS):
        p_list.append(p)
        q_list.append(q)
        p = ends[0, s : s + 1, :] * p + ends[1, s : s + 1, :]
        q = ends[0, s : s + 1, :] * q
    b = jnp.zeros((1, chan), F32)
    e = jnp.ones((1, chan), F32)
    for s in range(SUBS - 1, -1, -1):
        b_list[s] = b
        e_list[s] = e
        b = ends[0, s : s + 1, :] * b + ends[2, s : s + 1, :]
        e = ends[0, s : s + 1, :] * e
    car_out[0:1, :] = q
    car_out[1:2, :] = p
    car_out[2:3, :] = b
    car_out[3:8, :] = jnp.zeros((5, chan), F32)

    def car_copy(j):
        return pltpu.make_async_remote_copy(
            src_ref=car_out, dst_ref=car_in.at[j], send_sem=car_send.at[j],
            recv_sem=car_recv.at[j], device_id=(sp_at(j), tp), device_id_type=MESH,
        )

    def car_start(j, _):
        car_copy(j).start()
        return 0

    def car_wait(j, _):
        car_copy(j).wait()
        return 0

    lax.fori_loop(1, sp_n, car_start, 0)
    lax.fori_loop(1, sp_n, car_wait, 0)

    def join(m, state):
        cs, cg = state
        j = sp_n - m
        cs = jnp.where(j <= sp, car_in[j, 0:1, :] * cs + car_in[j, 1:2, :], cs)
        cg = jnp.where(sp + j < sp_n, car_in[m, 0:1, :] * cg + car_in[m, 2:3, :], cg)
        return cs, cg

    nothing = jnp.zeros((1, chan), F32)
    cs, cg = lax.fori_loop(1, sp_n, join, (nothing, nothing))
    for s in range(SUBS):
        carry_k[s] = p_list[s] + q_list[s] * cs
        carry_l[s] = b_list[s] + e_list[s] * cg

    def back(s):
        base = pl.multiple_of(s * pitch, PAD)
        outb = pl.multiple_of(s * sub_rows, STEP)
        for r in range(0, sub_rows, STEP):
            at = pl.ds(base + r, STEP)
            to = pl.ds(outb + r, STEP)
            for h in range(halves):
                lane = slice(h * LANES, (h + 1) * LANES)
                kk = carry_k[s, :, lane]
                ll = carry_l[s, :, lane]
                d = dec[h, at, :]
                prev = xp[h, at, :] + cp[h, at, :] * kk
                dp = d * prev
                dgate_ref[to, lane] = (qg[h, at, :] * (dp + drv[h, at, :])).astype(BF16)
                sg = gs[h, at, :] + as_[h, at, :] * ll
                ro, io, cv, sc = ro_s[h, at, :], io_s[h, at, :], cv_s[h, at, :], sc_s[h, at, :]
                dld = sg * (dp - io * cv * d * d * rs_s[h, at, :])
                dr = dld * slope_s[:, lane] * ro * (1.0 - ro)
                sgi = sg * sc * io
                di = sgi * cv * (1.0 - io)
                dri[r : r + STEP, lane] = dr.astype(BF16)
                dri[r : r + STEP, chan + h * LANES : chan + (h + 1) * LANES] = di.astype(BF16)
                dc[to, lane] = sgi
        whole = pl.ds(outb, sub_rows)
        dc[whole, :] += mm(dri[0:sub_rows, :], wblk[...], (((1,), (1,)), ((), ())))

    back(0)
    halo_out[...] = dc[0:PAD, :]
    dc_copy = pltpu.make_async_remote_copy(
        src_ref=halo_out, dst_ref=dc_in, send_sem=dc_send, recv_sem=dc_recv,
        device_id=(sp_at(sp_n - 1), tp), device_id_type=MESH,
    )
    dc_copy.start()

    def back_step(s, _):
        back(s)
        return 0

    lax.fori_loop(1, SUBS, back_step, 0)
    dc_copy.wait()
    dc[rows : rows + PAD, :] = jnp.where(sp < sp_n - 1, dc_in[...], 0.0)

    def unconv(i, _):
        r = pl.multiple_of(i * STEP, STEP)
        x = dc[pl.ds(r, STEP + PAD), :]
        total = taps_s[0:1, :] * x[:STEP]
        for k in range(1, 4):
            total = total + taps_s[k : k + 1, :] * pltpu.roll(x, STEP + PAD - k, 0)[:STEP]
        dproj_ref[pl.ds(r, STEP), :] = total.astype(BF16)
        return 0

    lax.fori_loop(0, rows // STEP, unconv, 0, unroll=4)

    piece = feat * tp_n // sp_n
    per = feat // piece
    paired = piece % LANES == 0 and sp_n % 2 == 0
    duos = sp_n // 2
    side = lax.rem(sp, 2)
    duo = lax.div(sp, 2)

    def slot_of(shard):
        behind = lax.rem(chip + chips - lax.div(shard, 2), chips)
        return 2 * behind + lax.rem(lax.rem(shard, 2) + core, 2)

    def rs_move(source, landing, target):
        return pltpu.make_async_remote_copy(
            src_ref=sbuf.at[source], dst_ref=rbuf.at[landing],
            send_sem=rs_send.at[landing], recv_sem=rs_recv.at[landing],
            device_id=(target, tp), device_id_type=MESH,
        )

    def rs_near(m):
        return rs_move(duos + m, duos + m, sp + 1 - 2 * side)

    def rs_far(m):
        if paired:
            return rs_move(m, m, lax.rem(duo + m, duos) * 2 + side)
        return rs_move(sp_at(m), m, sp_at(m))

    if paired:
        dpt[...] = dproj_ref[...].T

        def share(m, half):
            dest = lax.rem(duo + m, duos) * 2 + half
            x = gath[
                slot_of(lax.div(dest, per)), :, :,
                pl.ds(pl.multiple_of(lax.rem(dest, per) * piece, LANES), piece),
            ]
            return mm(dpt[...], x.reshape(rows, piece))

        def near_start(i, _):
            m = lax.rem(i + 1, duos)
            sbuf[duos + m] = share(m, 1 - side).astype(BF16)
            rs_near(m).start()
            return 0

        lax.fori_loop(0, duos, near_start, 0)

        def far_start(m, _):
            own[...] = share(m, side)
            rs_near(m).wait_recv()
            sbuf[m] = (own[...] + rbuf[duos + m].astype(F32)).astype(BF16)
            rs_far(m).start()
            return 0

        lax.fori_loop(1, duos, far_start, 0)
        own[...] = share(0, side)
        rs_near(0).wait_recv()
        own[...] += rbuf[duos].astype(F32)

        def near_drain(m, _):
            rs_near(m).wait_send()
            return 0

        lax.fori_loop(0, duos, near_drain, 0)
        peers = duos
    else:

        def shares(shard, _):
            x = gath[slot_of(shard)].reshape(rows, feat)
            full = mm(x, dproj_ref[...], (((0,), (0,)), ((), ())))
            sbuf[pl.ds(shard * per, per)] = full.astype(BF16).reshape(per, piece, chan)
            return 0

        lax.fori_loop(0, tp_n, shares, 0)

        def far_start(m, _):
            rs_far(m).start()
            return 0

        lax.fori_loop(1, sp_n, far_start, 0)
        own[...] = sbuf[sp].astype(F32)
        peers = sp_n

    def ag_drain(c, _):
        for j in range(chips):
            if j:
                cross(j, c).wait_send()
            inside(j, c).wait_send()
        return 0

    lax.fori_loop(0, chunks, ag_drain, 0)

    def rs_wait(j, _):
        rs_far(j).wait()
        return 0

    lax.fori_loop(1, peers, rs_wait, 0)
    height = own.shape[0]
    tile = min(32, height)

    def add(i, _):
        at = pl.ds(pl.multiple_of(i * tile, tile), tile)

        def more(j, acc):
            return acc + rbuf[j, at, :].astype(F32)

        own[at, :] = lax.fori_loop(1, peers, more, own[at, :])
        return 0

    lax.fori_loop(0, height // tile, add, 0)
    dw_ref[...] = own[...].T if paired else own[...]


def emit(*refs):
    sources, targets, rooms = refs[0:3], refs[3:6], refs[6:9]
    in_sem, out_sem = refs[9:]
    ins = [pltpu.make_async_copy(sources[i], rooms[i], in_sem.at[i]) for i in range(3)]
    outs = [pltpu.make_async_copy(rooms[i], targets[i], out_sem.at[i]) for i in range(3)]
    for item in ins:
        item.start()
    for i in range(3):
        ins[i].wait()
        outs[i].start()
    for item in outs:
        item.wait()


def per_device(
    tokens, proj_weight, gate_weight, conv_weight, recur_weight, input_weight, decay_param, out_grad
):
    sp_n = lax.axis_size("sp")
    tp_n = lax.axis_size("tp")
    rows, feat = tokens.shape
    width, chan = proj_weight.shape
    sub_rows = rows // SUBS
    chunks = sub_rows // STEP
    halves = chan // LANES
    pitch = sub_rows + PAD
    piece = width // sp_n
    box = (chan, piece) if piece % LANES == 0 and sp_n % 2 == 0 else (piece, chan)
    V = pltpu.VMEM
    DMA = pltpu.SemaphoreType.DMA
    tall = V((halves, SUBS * pitch, LANES), F32)
    small = V((PAD, chan), F32)
    any_space = pl.BlockSpec(memory_space=pl.ANY)
    in_vmem = pl.BlockSpec(memory_space=V)
    results = pl.pallas_call(
        functools.partial(kernel, sp_n=sp_n, tp_n=tp_n),
        out_shape=(
            jax.ShapeDtypeStruct((rows, chan), BF16),
            jax.ShapeDtypeStruct((rows, chan), BF16),
            jax.ShapeDtypeStruct((piece, chan), F32),
        ),
        in_specs=[any_space] * 3 + [in_vmem] * 4 + [any_space],
        out_specs=(in_vmem,) * 3,
        scratch_shapes=[
            V((tp_n, SUBS, sub_rows, feat), BF16),
            V((width, chan), BF16),
            V((width, chan), BF16),
            V((rows, chan), BF16),
            V((chan, 2 * chan), BF16),
            V((SUBS, pitch, chan), F32),
            V((SUBS, sub_rows, chan), F32),
            V((SUBS * STEP, 2 * chan), F32),
        ] + [tall] * 13 + [
            V((3, SUBS, chan), F32),
            V((SUBS, 1, chan), F32),
            V((SUBS, 1, chan), F32),
            V((1, chan), F32),
            V((4, chan), F32),
            small,
            small,
            small,
            V((sp_n, PAD, chan), F32),
            V((max(SUBS * STEP, sub_rows), 2 * chan), BF16),
            V((rows + PAD, chan), F32),
            small,
            V((chan, rows), BF16),
            V((sp_n,) + box, BF16),
            V((sp_n,) + box, BF16),
            V(box, F32),
            DMA((4,)),
            DMA((tp_n, chunks)), DMA((tp_n, chunks)),
            DMA, DMA,
            DMA((sp_n,)), DMA((sp_n,)),
            DMA, DMA,
            DMA((sp_n,)), DMA((sp_n,)),
        ],
        compiler_params=pltpu.CompilerParams(
            collective_id=0, has_side_effects=True, vmem_limit_bytes=56 * 1024 * 1024
        ),
    )(
        tokens.reshape(SUBS, sub_rows, feat), proj_weight, gate_weight, conv_weight,
        recur_weight, input_weight, decay_param.reshape(1, -1), out_grad,
    )
    shapes = [jax.ShapeDtypeStruct(r.shape, r.dtype) for r in results]
    return pl.pallas_call(
        emit,
        out_shape=tuple(shapes),
        in_specs=[any_space] * 3,
        out_specs=(any_space,) * 3,
        scratch_shapes=[V(s.shape, s.dtype) for s in shapes] + [DMA((3,)), DMA((3,))],
    )(*results)


def solution(mesh):
    in_specs = (P("sp", "tp"), P(None, "tp"), P(None, "tp"), P(), P(), P(), P(), P("sp", "tp"))
    out_specs = (P("sp", "tp"), P("sp", "tp"), P("sp", "tp"))
    return jax.shard_map(
        per_device, mesh=mesh, in_specs=in_specs, out_specs=out_specs, check_vma=False
    )
```

```python
import functools

import jax
import jax.numpy as jnp
from jax import lax
from jax.experimental import pallas as pl
from jax.experimental.pallas import tpu as pltpu
from jax.sharding import PartitionSpec as P

BLOCK = 64
rate_scale = 8.0
scale_floor = 0.0001

SUBS = 8
PARTS = 4
STEP = 16
LANES = 128
PAD = 8
MESH = pl.DeviceIdType.MESH
F32 = jnp.float32
BF16 = jnp.bfloat16


def mm(a, b, dims=(((1,), (0,)), ((), ()))):
    return lax.dot_general(a, b, dims, preferred_element_type=F32)


def kernel(
    tok_hbm, wp_hbm, wg_hbm, cw_ref, wr_ref, wi_ref, dp_ref, og_hbm,
    dproj_hbm, dgate_hbm, dw_ref,
    gath, wp, wg, og, wblk, proj, gin, pre,
    dec, drv, dgr, qg, ro_s, io_s, cv_s, sc_s, rs_s, xp, cp, gs, as_,
    ends, carry_k, carry_l, slope_s, taps_s,
    halo_out, halo_in, car_out, car_in, dri, dc, dc_in, dpt, sbuf, rbuf, own,
    loc_sem, ag_send, ag_recv, halo_send, halo_recv, car_send, car_recv,
    dc_send, dc_recv, rs_send, rs_recv, dproj_ref, dgate_ref, out_sem,
    *, sp_n, tp_n,
):
    sp = lax.axis_index("sp")
    tp = lax.axis_index("tp")
    core = lax.rem(tp, 2)
    chip = lax.div(tp, 2)
    chips = tp_n // 2
    partner = tp + 1 - 2 * core
    sub_rows = gath.shape[2]
    feat = gath.shape[3]
    chan = wp.shape[1]
    halves = chan // LANES
    pitch = sub_rows + PAD
    chunks = sub_rows // STEP
    rows = SUBS * sub_rows
    groups = chan // BLOCK

    loc = [
        pltpu.make_async_copy(tok_hbm, gath.at[0], loc_sem.at[0]),
        pltpu.make_async_copy(wp_hbm, wp, loc_sem.at[1]),
        pltpu.make_async_copy(wg_hbm, wg, loc_sem.at[2]),
        pltpu.make_async_copy(og_hbm, og, loc_sem.at[3]),
    ]
    for item in loc:
        item.start()

    def sp_at(j):
        return lax.rem(sp + j, sp_n)

    def chip_at(j):
        return lax.rem(chip + j, chips)

    barrier = pltpu.get_barrier_semaphore()
    pl.semaphore_signal(barrier, inc=1, device_id=(sp, partner), device_id_type=MESH)
    for j in range(1, chips):
        pl.semaphore_signal(
            barrier, inc=1, device_id=(sp, chip_at(j) * 2 + core), device_id_type=MESH
        )

    def greet(j, _):
        pl.semaphore_signal(barrier, inc=1, device_id=(sp_at(j), tp), device_id_type=MESH)
        return 0

    lax.fori_loop(1, sp_n, greet, 0)

    cols = pl.ds(pl.multiple_of(tp * chan, chan), chan)
    z = jnp.exp(-dp_ref[:, cols])
    log1p = z * (1.0 - z * (1.0 / 2 - z * (1.0 / 3 - z * (1.0 / 4 - z * (1.0 / 5)))))
    slope_s[...] = -rate_scale * log1p
    taps_s[...] = cw_ref[:, cols]
    wblk[...] = jnp.zeros_like(wblk)
    for g in range(groups):
        at = slice(g * BLOCK, (g + 1) * BLOCK)
        wblk[at, at] = wr_ref[tp * groups + g]
        wblk[at, chan + g * BLOCK : chan + (g + 1) * BLOCK] = wi_ref[tp * groups + g]

    pl.semaphore_wait(barrier, chips + sp_n - 1)
    loc[0].wait()

    def part(c):
        return pl.ds(pl.multiple_of(c * STEP, STEP), STEP)

    def ag_copy(slot, source, c, target):
        return pltpu.make_async_remote_copy(
            src_ref=gath.at[source, :, part(c), :],
            dst_ref=gath.at[slot, :, part(c), :],
            send_sem=ag_send.at[slot, c],
            recv_sem=ag_recv.at[slot, c],
            device_id=(sp, target),
            device_id_type=MESH,
        )

    def cross(j, c):
        return ag_copy(2 * j, 0, c, chip_at(j) * 2 + core)

    def inside(j, c):
        return ag_copy(2 * j + 1, 2 * j, c, partner)

    def send_own(k, _):
        c = lax.rem(k + chunks - 1, chunks)
        for j in range(1, chips):
            cross(j, c).start()
        inside(0, c).start()
        return 0

    lax.fori_loop(0, chunks, send_own, 0)
    for item in loc[1:]:
        item.wait()

    def relay(c):
        for j in range(1, chips):
            cross(j, c).wait_recv()
            inside(j, c).start()

    def project(c):
        acc_p = acc_g = None
        for j in range(chips):
            for other in range(2):
                rel = 2 * j + other
                if other:
                    inside(j, c).wait_recv()
                shard = lax.rem(chip + chips - j, chips) * 2 + (1 - core if other else core)
                x = gath[rel, :, part(c), :].reshape(SUBS * STEP, feat)
                wrows = pl.ds(pl.multiple_of(shard * feat, feat), feat)
                a = mm(x, wp[wrows, :])
                b = mm(x, wg[wrows, :])
                acc_p = a if acc_p is None else acc_p + a
                acc_g = b if acc_g is None else acc_g + b
        shape = (SUBS, STEP, chan)
        proj[:, pl.ds(pl.multiple_of(c * STEP + PAD, PAD), STEP), :] = (
            acc_p.astype(BF16).astype(F32).reshape(shape)
        )
        gin[:, part(c), :] = acc_g.astype(BF16).astype(F32).reshape(shape)

    def gates(c):
        def conv(s, _):
            x = proj[s, pl.ds(pl.multiple_of(c * STEP, PAD), STEP + PAD), :]
            total = taps_s[0:1, :] * x[PAD:]
            for k in range(1, 4):
                total = total + taps_s[k : k + 1, :] * pltpu.roll(x, k, 0)[PAD:]
            dri[pl.ds(pl.multiple_of(s * STEP, STEP), STEP), 0:chan] = total.astype(BF16)
            return 0

        lax.fori_loop(0, SUBS, conv, 0, unroll=4)
        pre[...] = mm(dri[0 : SUBS * STEP, 0:chan], wblk[...])

        def element(s, _):
            at = pl.ds(pl.multiple_of(s * STEP, STEP), STEP)
            to = pl.ds(pl.multiple_of(s * pitch + c * STEP, PAD), STEP)
            src = pl.ds(pl.multiple_of(s * sub_rows + c * STEP, STEP), STEP)
            for h in range(halves):
                lane = slice(h * LANES, (h + 1) * LANES)
                slope = slope_s[:, lane]
                cv = dri[at, lane].astype(F32)
                ro = 0.5 * jnp.tanh(0.5 * pre[at, lane]) + 0.5
                io = 0.5 * jnp.tanh(0.5 * pre[at, chan + h * LANES : chan + (h + 1) * LANES]) + 0.5
                ld = slope * ro
                d = jnp.exp(ld)
                y = 2.0 * ld
                poly = 1.0 + y * (1.0 / 8)
                for m in range(7, 1, -1):
                    poly = 1.0 + (y * (1.0 / m)) * poly
                u = scale_floor - y * poly
                rs = lax.rsqrt(u)
                sc = u * rs
                x = gin[s, part(c), lane]
                cot = og[src, lane].astype(F32)
                x2 = x * x
                th = jnp.tanh(0.7978845608028654 * (x + 0.044715 * (x2 * x)))
                half_up = 0.5 * (1.0 + th)
                slope_g = half_up + 0.5 * x * (1.0 - th * th) * (
                    0.7978845608028654 * (1.0 + 0.134145 * x2)
                )
                dec[h, to, :] = d
                drv[h, to, :] = sc * (io * cv)
                dgr[h, to, :] = cot * (x * half_up)
                qg[h, to, :] = cot * slope_g
                ro_s[h, to, :] = ro
                io_s[h, to, :] = io
                cv_s[h, to, :] = cv
                sc_s[h, to, :] = sc
                rs_s[h, to, :] = rs
            return 0

        lax.fori_loop(0, SUBS, element, 0, unroll=4)

    halo = pltpu.make_async_remote_copy(
        src_ref=halo_out, dst_ref=halo_in, send_sem=halo_send, recv_sem=halo_recv,
        device_id=(sp_at(1), tp), device_id_type=MESH,
    )
    relay(chunks - 1)
    project(chunks - 1)
    halo_out[...] = proj[SUBS - 1, sub_rows:pitch, :]
    halo.start()
    for s in range(1, SUBS):
        proj[s, 0:PAD, :] = proj[s - 1, sub_rows:pitch, :]
    relay(0)
    project(0)
    halo.wait()
    proj[0, 0:PAD, :] = jnp.where(sp > 0, halo_in[...], 0.0)

    def stream(c, _):
        relay(c)
        gates(c - 1)
        project(c)
        return 0

    lax.fori_loop(1, chunks - 1, stream, 0)

    def rest(c, _):
        gates(c)
        return 0

    lax.fori_loop(chunks - 2, chunks, rest, 0)

    one = jnp.ones((SUBS, LANES), F32)
    zero = jnp.zeros((SUBS, LANES), F32)

    def scan(i, state):
        out = []
        fwd = pl.ds(i, SUBS, stride=pitch)
        rev = pl.ds(sub_rows - 1 - i, SUBS, stride=pitch)
        for h in range(halves):
            x, c, g, a = state[4 * h : 4 * h + 4]
            d = dec.at[h][fwd, :]
            xp.at[h][fwd, :] = x
            cp.at[h][fwd, :] = c
            x = d * x + drv.at[h][fwd, :]
            c = c * d
            e = dec.at[h][rev, :]
            g = g + dgr.at[h][rev, :]
            gs.at[h][rev, :] = g
            as_.at[h][rev, :] = a
            g = e * g
            a = a * e
            out += [x, c, g, a]
        return tuple(out)

    final = lax.fori_loop(0, sub_rows, scan, (zero, one, zero, one) * halves, unroll=4)
    for h in range(halves):
        lane = slice(h * LANES, (h + 1) * LANES)
        ends[0, :, lane] = final[4 * h + 1]
        ends[1, :, lane] = final[4 * h]
        ends[2, :, lane] = final[4 * h + 2]
    p_list, q_list, b_list, e_list = [], [], [None] * SUBS, [None] * SUBS
    p = jnp.zeros((1, chan), F32)
    q = jnp.ones((1, chan), F32)
    for s in range(SUBS):
        p_list.append(p)
        q_list.append(q)
        p = ends[0, s : s + 1, :] * p + ends[1, s : s + 1, :]
        q = ends[0, s : s + 1, :] * q
    b = jnp.zeros((1, chan), F32)
    e = jnp.ones((1, chan), F32)
    for s in range(SUBS - 1, -1, -1):
        b_list[s] = b
        e_list[s] = e
        b = ends[0, s : s + 1, :] * b + ends[2, s : s + 1, :]
        e = ends[0, s : s + 1, :] * e
    car_out[0:1, :] = q
    car_out[1:2, :] = p
    car_out[2:3, :] = b
    car_out[3:8, :] = jnp.zeros((5, chan), F32)

    def car_copy(j):
        return pltpu.make_async_remote_copy(
            src_ref=car_out, dst_ref=car_in.at[j], send_sem=car_send.at[j],
            recv_sem=car_recv.at[j], device_id=(sp_at(j), tp), device_id_type=MESH,
        )

    def car_start(j, _):
        car_copy(j).start()
        return 0

    def car_wait(j, _):
        car_copy(j).wait()
        return 0

    lax.fori_loop(1, sp_n, car_start, 0)
    lax.fori_loop(1, sp_n, car_wait, 0)

    def join(m, state):
        cs, cg = state
        j = sp_n - m
        cs = jnp.where(j <= sp, car_in[j, 0:1, :] * cs + car_in[j, 1:2, :], cs)
        cg = jnp.where(sp + j < sp_n, car_in[m, 0:1, :] * cg + car_in[m, 2:3, :], cg)
        return cs, cg

    nothing = jnp.zeros((1, chan), F32)
    cs, cg = lax.fori_loop(1, sp_n, join, (nothing, nothing))
    for s in range(SUBS):
        carry_k[s] = p_list[s] + q_list[s] * cs
        carry_l[s] = b_list[s] + e_list[s] * cg

    def back(s):
        base = pl.multiple_of(s * pitch, PAD)
        outb = pl.multiple_of(s * sub_rows, STEP)
        for r in range(0, sub_rows, STEP):
            at = pl.ds(base + r, STEP)
            to = pl.ds(outb + r, STEP)
            for h in range(halves):
                lane = slice(h * LANES, (h + 1) * LANES)
                kk = carry_k[s, :, lane]
                ll = carry_l[s, :, lane]
                d = dec[h, at, :]
                prev = xp[h, at, :] + cp[h, at, :] * kk
                dp = d * prev
                dgate_ref[to, lane] = (qg[h, at, :] * (dp + drv[h, at, :])).astype(BF16)
                sg = gs[h, at, :] + as_[h, at, :] * ll
                ro, io, cv, sc = ro_s[h, at, :], io_s[h, at, :], cv_s[h, at, :], sc_s[h, at, :]
                dld = sg * (dp - io * cv * d * d * rs_s[h, at, :])
                dr = dld * slope_s[:, lane] * ro * (1.0 - ro)
                sgi = sg * sc * io
                di = sgi * cv * (1.0 - io)
                dri[r : r + STEP, lane] = dr.astype(BF16)
                dri[r : r + STEP, chan + h * LANES : chan + (h + 1) * LANES] = di.astype(BF16)
                dc[to, lane] = sgi
        whole = pl.ds(outb, sub_rows)
        dc[whole, :] += mm(dri[0:sub_rows, :], wblk[...], (((1,), (1,)), ((), ())))

    back(0)
    halo_out[...] = dc[0:PAD, :]
    dc_copy = pltpu.make_async_remote_copy(
        src_ref=halo_out, dst_ref=dc_in, send_sem=dc_send, recv_sem=dc_recv,
        device_id=(sp_at(sp_n - 1), tp), device_id_type=MESH,
    )
    dc_copy.start()

    def back_step(s, _):
        back(s)
        return 0

    lax.fori_loop(1, SUBS, back_step, 0)
    dc_copy.wait()
    dc[rows : rows + PAD, :] = jnp.where(sp < sp_n - 1, dc_in[...], 0.0)

    def unconv(i, _):
        r = pl.multiple_of(i * STEP, STEP)
        x = dc[pl.ds(r, STEP + PAD), :]
        total = taps_s[0:1, :] * x[:STEP]
        for k in range(1, 4):
            total = total + taps_s[k : k + 1, :] * pltpu.roll(x, STEP + PAD - k, 0)[:STEP]
        dproj_ref[pl.ds(r, STEP), :] = total.astype(BF16)
        return 0

    lax.fori_loop(0, rows // STEP, unconv, 0, unroll=4)

    leave = [
        pltpu.make_async_copy(dproj_ref, dproj_hbm, out_sem.at[0]),
        pltpu.make_async_copy(dgate_ref, dgate_hbm, out_sem.at[1]),
    ]
    for item in leave:
        item.start()

    piece = feat * tp_n // sp_n
    per = feat // piece
    paired = piece % LANES == 0 and sp_n % 2 == 0
    duos = sp_n // 2
    side = lax.rem(sp, 2)
    duo = lax.div(sp, 2)

    def slot_of(shard):
        behind = lax.rem(chip + chips - lax.div(shard, 2), chips)
        return 2 * behind + lax.rem(lax.rem(shard, 2) + core, 2)

    cuts = PARTS if paired else 1
    slab = own.shape[0] // cuts

    def rs_move(source, landing, target, cut):
        across = pl.ds(cut * slab, slab)
        return pltpu.make_async_remote_copy(
            src_ref=sbuf.at[source, across], dst_ref=rbuf.at[landing, across],
            send_sem=rs_send.at[landing, cut], recv_sem=rs_recv.at[landing, cut],
            device_id=(target, tp), device_id_type=MESH,
        )

    def rs_near(m, cut):
        return rs_move(duos + m, duos + m, sp + 1 - 2 * side, cut)

    def rs_far(m, cut):
        if paired:
            return rs_move(m, m, lax.rem(duo + m, duos) * 2 + side, cut)
        return rs_move(sp_at(m), m, sp_at(m), cut)

    if paired:
        dpt[...] = dproj_ref[...].T

        def share(m, half):
            dest = lax.rem(duo + m, duos) * 2 + half
            x = gath[
                slot_of(lax.div(dest, per)), :, :,
                pl.ds(pl.multiple_of(lax.rem(dest, per) * piece, LANES), piece),
            ]
            return mm(dpt[...], x.reshape(rows, piece))

        def near_start(i, _):
            m = lax.rem(i + 1, duos)
            sbuf[duos + m] = share(m, 1 - side).astype(BF16)
            for cut in range(cuts):
                rs_near(m, cut).start()
            return 0

        lax.fori_loop(0, duos, near_start, 0)

        def far_start(m, _):
            own[...] = share(m, side)
            for cut in range(cuts):
                across = pl.ds(cut * slab, slab)
                rs_near(m, cut).wait_recv()
                sbuf[m, across] = (own[across] + rbuf[duos + m, across].astype(F32)).astype(BF16)
                rs_far(m, cut).start()
            return 0

        lax.fori_loop(1, duos, far_start, 0)
        own[...] = share(0, side)
        for cut in range(cuts):
            rs_near(0, cut).wait_recv()
        own[...] += rbuf[duos].astype(F32)

        def near_drain(m, _):
            for cut in range(cuts):
                rs_near(m, cut).wait_send()
            return 0

        lax.fori_loop(0, duos, near_drain, 0)
        peers = duos
    else:

        def shares(shard, _):
            x = gath[slot_of(shard)].reshape(rows, feat)
            full = mm(x, dproj_ref[...], (((0,), (0,)), ((), ())))
            sbuf[pl.ds(shard * per, per)] = full.astype(BF16).reshape(per, piece, chan)
            return 0

        lax.fori_loop(0, tp_n, shares, 0)

        def far_start(m, _):
            rs_far(m, 0).start()
            return 0

        lax.fori_loop(1, sp_n, far_start, 0)
        own[...] = sbuf[sp].astype(F32)
        peers = sp_n

    def ag_drain(c, _):
        for j in range(chips):
            if j:
                cross(j, c).wait_send()
            inside(j, c).wait_send()
        return 0

    lax.fori_loop(0, chunks, ag_drain, 0)

    def rs_wait(j, _):
        for cut in range(cuts):
            rs_far(j, cut).wait()
        return 0

    lax.fori_loop(1, peers, rs_wait, 0)
    height = own.shape[0]
    tile = min(32, height)

    def add(i, _):
        at = pl.ds(pl.multiple_of(i * tile, tile), tile)

        def more(j, acc):
            return acc + rbuf[j, at, :].astype(F32)

        own[at, :] = lax.fori_loop(1, peers, more, own[at, :])
        return 0

    lax.fori_loop(0, height // tile, add, 0)
    for item in leave:
        item.wait()
    dw_ref[...] = own[...].T if paired else own[...]


def emit(*refs):
    sources, targets, rooms = refs[0:3], refs[3:6], refs[6:9]
    in_sem, out_sem = refs[9:]
    ins = [pltpu.make_async_copy(sources[i], rooms[i], in_sem.at[i]) for i in range(3)]
    outs = [pltpu.make_async_copy(rooms[i], targets[i], out_sem.at[i]) for i in range(3)]
    for item in ins:
        item.start()
    for i in range(3):
        ins[i].wait()
        outs[i].start()
    for item in outs:
        item.wait()


def per_device(
    tokens, proj_weight, gate_weight, conv_weight, recur_weight, input_weight, decay_param, out_grad
):
    sp_n = lax.axis_size("sp")
    tp_n = lax.axis_size("tp")
    rows, feat = tokens.shape
    width, chan = proj_weight.shape
    sub_rows = rows // SUBS
    chunks = sub_rows // STEP
    halves = chan // LANES
    pitch = sub_rows + PAD
    piece = width // sp_n
    box = (chan, piece) if piece % LANES == 0 and sp_n % 2 == 0 else (piece, chan)
    V = pltpu.VMEM
    DMA = pltpu.SemaphoreType.DMA
    tall = V((halves, SUBS * pitch, LANES), F32)
    small = V((PAD, chan), F32)
    any_space = pl.BlockSpec(memory_space=pl.ANY)
    in_vmem = pl.BlockSpec(memory_space=V)
    results = pl.pallas_call(
        functools.partial(kernel, sp_n=sp_n, tp_n=tp_n),
        out_shape=(
            jax.ShapeDtypeStruct((rows, chan), BF16),
            jax.ShapeDtypeStruct((rows, chan), BF16),
            jax.ShapeDtypeStruct((piece, chan), F32),
        ),
        in_specs=[any_space] * 3 + [in_vmem] * 4 + [any_space],
        out_specs=(any_space, any_space, in_vmem),
        scratch_shapes=[
            V((tp_n, SUBS, sub_rows, feat), BF16),
            V((width, chan), BF16),
            V((width, chan), BF16),
            V((rows, chan), BF16),
            V((chan, 2 * chan), BF16),
            V((SUBS, pitch, chan), F32),
            V((SUBS, sub_rows, chan), F32),
            V((SUBS * STEP, 2 * chan), F32),
        ] + [tall] * 13 + [
            V((3, SUBS, chan), F32),
            V((SUBS, 1, chan), F32),
            V((SUBS, 1, chan), F32),
            V((1, chan), F32),
            V((4, chan), F32),
            small,
            small,
            small,
            V((sp_n, PAD, chan), F32),
            V((max(SUBS * STEP, sub_rows), 2 * chan), BF16),
            V((rows + PAD, chan), F32),
            small,
            V((chan, rows), BF16),
            V((sp_n,) + box, BF16),
            V((sp_n,) + box, BF16),
            V(box, F32),
            DMA((4,)),
            DMA((tp_n, chunks)), DMA((tp_n, chunks)),
            DMA, DMA,
            DMA((sp_n,)), DMA((sp_n,)),
            DMA, DMA,
            DMA((sp_n, PARTS)), DMA((sp_n, PARTS)),
            V((rows, chan), BF16),
            V((rows, chan), BF16),
            DMA((2,)),
        ],
        compiler_params=pltpu.CompilerParams(
            collective_id=0, has_side_effects=True, vmem_limit_bytes=56 * 1024 * 1024
        ),
    )(
        tokens.reshape(SUBS, sub_rows, feat), proj_weight, gate_weight, conv_weight,
        recur_weight, input_weight, decay_param.reshape(1, -1), out_grad,
    )
    shapes = [jax.ShapeDtypeStruct(r.shape, r.dtype) for r in results]
    return pl.pallas_call(
        emit,
        out_shape=tuple(shapes),
        in_specs=[any_space] * 3,
        out_specs=(any_space,) * 3,
        scratch_shapes=[V(s.shape, s.dtype) for s in shapes] + [DMA((3,)), DMA((3,))],
    )(*results)


def solution(mesh):
    in_specs = (P("sp", "tp"), P(None, "tp"), P(None, "tp"), P(), P(), P(), P(), P("sp", "tp"))
    out_specs = (P("sp", "tp"), P("sp", "tp"), P("sp", "tp"))
    return jax.shard_map(
        per_device, mesh=mesh, in_specs=in_specs, out_specs=out_specs, check_vma=False
    )
```
